32 devices in a mesh: sp: 8 (over z, y), tp: 4 (over x, core).
Axes of the slice: x: 2, y: 2, z: 4, core: 2. Of those that a mesh axis runs over, the one named last changes fastest.
Arguments:
- cotangent: bfloat16 [1280, 2048], P('sp'), may hold values from -8 to 8
- saved_input: bfloat16 [1280, 2048], P('sp'), may hold values from -200 to 200
- routes: int32 [1280, 2], P('sp'), may hold values from 0 to 7, all different within a row; in each aligned block of 160 rows (0 to 159, 160 to 319, ...) at most 80 rows name the same one
- route_weight: float32 [1280, 2], P('sp'), may hold values from 0.2 to 1.5
- gate_proj: bfloat16 [8, 2048, 1024], P('sp', None, 'tp'), may hold values from -0.125 to 0.125
- up_proj: bfloat16 [8, 2048, 1024], P('sp', None, 'tp'), may hold values from -0.125 to 0.125
- down_proj: bfloat16 [8, 1024, 2048], P('sp', 'tp'), may hold values from -0.1875 to 0.1875
- out_proj: bfloat16 [2048, 1024], P(None, 'tp'), may hold values from -0.1875 to 0.1875
- conv_input: bfloat16 [1280, 1024], P('sp', 'tp'), may hold values from -6 to 6
- gate_branch: bfloat16 [1280, 1024], P('sp', 'tp'), may hold values from -6 to 6
- conv_taps: bfloat16 [4, 1024], P(None, 'tp'), may hold values from -3 to 3
- recur_map: bfloat16 [2, 16, 64, 64], P(None, 'tp'), may hold values from -0.75 to 0.75
- input_map: bfloat16 [2, 16, 64, 64], P(None, 'tp'), may hold values from -0.75 to 0.75
- decay_param: float32 [2, 1024], P(None, 'tp'), may hold values from 4 to 30
- decay_shift: float32 [2, 1280, 1024], P(None, 'sp', 'tp'), may hold values from -2 to 0, as said below
Outputs:
- grad_gate_proj: float32 [8, 2048, 1024], P('sp', None, 'tp')
- grad_up_proj: float32 [8, 2048, 1024], P('sp', None, 'tp')
- grad_down_proj: float32 [8, 1024, 2048], P('sp', 'tp')
- grad_out_proj: float32 [2048, 1024], P('sp', 'tp')
- grad_conv_input: bfloat16 [1280, 1024], P('sp', 'tp')
- grad_gate_branch: bfloat16 [1280, 1024], P('sp', 'tp')
The draws below stay inside these ranges and needn't reach their ends.
Inputs may be any that keep to these rules, and one draw needn't show every extreme that they name: Each row names 2 different experts; among the rows of one device no expert is named by more than 80 rows, and in every draw some device routes exactly 80 rows to some expert. `decay_shift`: together with decay_param, -log_decay stays at or above softplus(-decay_param) for every channel and position.
All inputs are finite; a program needn't handle non-finite values.
Results may differ from the reference program's by a relative error of at most 0.013.
Values may be sent and summed in bfloat16 or wider, within the bound.
A program may use at most 128 MiB of HBM per device.

```python
import math
import jax
import jax.numpy as jnp
import numpy as np
from jax import lax

D = 2048
F = 1024
SCAN_CHANNELS = 1024
HW = 64
CONV_W = 4
TOP_K = 2
TOK_DEV = 160
EXPERTS = 8
STEP_COUNT = 1280
CAP = 80
N_SP = 8
N_TP = 4


DECAY_SCALE = 8.0


def decay_rates(key):
    base = jax.random.fold_in(key, 11)
    keys = jax.random.split(base, 3)
    share = 0.5
    fast = jax.random.uniform(keys[0], (2, SCAN_CHANNELS), jnp.float32) < share
    slow_rate = jnp.exp(jax.random.uniform(keys[1], (2, SCAN_CHANNELS), jnp.float32, math.log(0.005), math.log(0.05))) / STEP_COUNT
    fast_rate = jnp.exp(jax.random.uniform(keys[2], (2, SCAN_CHANNELS), jnp.float32, math.log(0.0025), math.log(0.008)))
    return jnp.where(fast, fast_rate, slow_rate)


def draw_decay_param(key, part):
    rate = decay_rates(key)
    return (-jnp.log(jnp.expm1(rate))).astype(jnp.float32)


def draw_decay_shift(key, part):
    rate = decay_rates(key)
    keys = jax.random.split(jax.random.fold_in(key, 12), 3)
    blocks = STEP_COUNT // TOK_DEV
    pace = jnp.exp(jax.random.uniform(keys[0], (2, blocks, SCAN_CHANNELS), jnp.float32, math.log(1.25), math.log(4.0)))
    pace_rows = jnp.repeat(pace, TOK_DEV, axis=1)
    filtered_signal = -DECAY_SCALE * 0.5 * rate[:, None, :] * (pace_rows - 1.0)
    expert_seats = jax.random.randint(keys[1], (2, 2, SCAN_CHANNELS), 0, STEP_COUNT)
    stack_level = jax.random.uniform(keys[2], (2, 2, SCAN_CHANNELS), jnp.float32, 0.2, 0.45)
    step_location = jnp.arange(STEP_COUNT, dtype=jnp.int32)[None, :, None]
    tally_clusters = jnp.zeros((2, STEP_COUNT, SCAN_CHANNELS), jnp.float32)
    for step_number in range(2):
        tally_clusters = tally_clusters + jnp.where(step_location == expert_seats[:, step_number][:, None, :], jnp.log1p(-stack_level[:, step_number])[:, None, :], 0.0)
    return (filtered_signal + tally_clusters).astype(jnp.float32)


def draw_saved_input(key, part):
    keys = jax.random.split(jax.random.fold_in(key, 13), 4)
    noise = jnp.clip(jax.random.normal(keys[0], (STEP_COUNT, D), jnp.float32), -4.0, 4.0)
    mixed = noise
    row_scale = jnp.exp(jax.random.uniform(keys[2], (STEP_COUNT, 1), jnp.float32, math.log(0.5), math.log(5.0)))
    column_scale = jnp.exp(jax.random.uniform(keys[3], (1, D), jnp.float32, math.log(0.3), math.log(3.0)))
    return (mixed * row_scale * column_scale).astype(jnp.bfloat16)


def with_spikes(values, rng, source, target, shards_of, factor):
    def block_of(dim):
        return (jnp.arange(values.shape[dim]) // (values.shape[dim] // shards_of)).reshape((-1,) + (1,) * (values.ndim - 1 - dim))

    near = jax.random.permutation(rng, shards_of)[block_of(target)]
    other_side = (block_of(target) + shards_of // 2) % shards_of
    return jnp.where((block_of(source) == near) | (block_of(source) == other_side), factor * values, values)


def block_scale(own_key, shape, cuts, least, largest):
    def one(axis_at, parts):
        draws = jax.random.uniform(jax.random.fold_in(jax.random.fold_in(own_key, 6), axis_at), (parts,), jnp.float32, least / len(cuts), largest / len(cuts))
        return jnp.repeat(jnp.exp(draws), shape[axis_at] // parts).reshape((-1,) + (1,) * (len(shape) - axis_at - 1))

    loudness = one(*cuts[0])
    for cut in cuts[1:]:
        loudness = loudness * one(*cut)
    return loudness


def shared_out(rng, own, number, rows, amount, top, most, lean):
    sequence = jax.random.permutation(rng, amount)
    crowded, ordinary = load_shares(amount, rows * top, most, lean, True), load_shares(amount, rows * top, most, lean, False)
    places = jnp.arange(amount)

    def named(lengths, rotation):
        used = int((lengths > 0).sum())
        fixed = max(1, used // 4)
        passed = fixed + (places - fixed + rotation * (used - fixed)) % max(1, amount - fixed)
        return jnp.zeros((amount,), jnp.int32).at[sequence[jnp.where(places < fixed, places, passed)]].set(jnp.asarray(lengths, jnp.int32))

    lengths = jnp.where(number % 4 == 0, named(crowded, number // 4), named(ordinary, number - number // 4 - 1))
    mixed = jax.random.permutation(jax.random.fold_in(own, 3), amount)
    source_of, receiver = mixed[0:amount // 2 * 2:2], mixed[1:amount // 2 * 2:2]
    margin = jnp.minimum(lengths[source_of] - 1, most - lengths[receiver]) // 2
    margin = jnp.where((source_of == sequence[0]) | (receiver == sequence[0]) | (lengths[receiver] == 0), 0, jnp.maximum(margin, 0))
    passed = jax.random.randint(jax.random.fold_in(own, 4), (amount // 2,), 0, 1 << 20) % (margin + 1)
    lengths = lengths.at[source_of].add(-passed).at[receiver].add(passed)
    items = jnp.searchsorted(jnp.cumsum(lengths), jnp.arange(rows * top), side="right").astype(jnp.int32)
    grid = items.reshape(top, rows).T
    grid = grid[jax.random.permutation(jax.random.fold_in(own, 1), rows)]
    rotation = jax.random.randint(jax.random.fold_in(own, 2), (rows, 1), 0, top)
    return jnp.take_along_axis(grid, (jnp.arange(top)[None, :] + rotation) % top, axis=1)


def load_shares(amount, total, bound, skew, full):
    loads = [(1 << 20) // math.isqrt(grade ** skew) + 1 for grade in range(1, amount + 1)]
    largest = bound if full else min(bound, max(-(-total // amount), total * loads[0] // sum(loads)))
    least = 1 if total - largest >= amount - 1 else 0
    given, spare = [largest] + [least] * (amount - 1), total - largest - least * (amount - 1)
    while spare > 0:
        free = [i for i in range(1, amount) if given[i] < largest] or [i for i in range(1, amount) if given[i] < bound]
        pool, left = sum([loads[i] for i in free]), spare
        for i in free:
            more = min(bound - given[i], max(1, left * loads[i] // pool), spare)
            given[i] = given[i] + more
            spare = spare - more
    return np.array(given)


def bell_draw(rng, shape, spread, reach, cuts=(), kind=jnp.bfloat16):
    result = spread * jax.random.normal(rng, shape, jnp.float32)
    if cuts:
        result = result * block_scale(rng, shape, cuts, -0.22, 0.18)
    return jnp.clip(result, -reach, reach).astype(kind)


def bell_draw_with(rng, shape, deviation, most, cuts, heavy, kind=jnp.bfloat16):
    result = deviation * jax.random.normal(rng, shape, jnp.float32)
    if cuts:
        result = result * block_scale(rng, shape, cuts, -0.22, 0.18)
    return jnp.clip(with_spikes(result, jax.random.fold_in(rng, 3), *heavy), -most, most).astype(kind)


def setup_inputs(seed: int = 0) -> dict:
    key_list = jax.random.split(jax.random.key(seed), 16)
    cotangent = bell_draw_with(key_list[0], (STEP_COUNT, D), 1.0, 8.0, ((0, 8),), (0, 1, 8, 2.0))
    saved_input = draw_saved_input(jax.random.fold_in(key_list[15], 71), 0)
    routes_keys = jax.random.split(jax.random.fold_in(key_list[2], 1), STEP_COUNT // TOK_DEV)
    routes_turns = jax.random.permutation(jax.random.fold_in(key_list[2], 3), STEP_COUNT // TOK_DEV)
    routes = jax.vmap(lambda own, number: shared_out(jax.random.fold_in(key_list[2], 2), own, number, TOK_DEV, EXPERTS, TOP_K, CAP, 1))(routes_keys, routes_turns).reshape((STEP_COUNT, TOP_K))
    route_weight = jnp.clip(0.2 + 1.3 * jax.random.uniform(key_list[3], (STEP_COUNT, TOP_K), jnp.float32) ** block_scale(key_list[3], (STEP_COUNT, TOP_K), ((0, 8),), -0.2, 0.2), 0.2, 1.5)
    gate_proj = bell_draw(key_list[4], (EXPERTS, D, F), D ** -0.5, 0.125, ((0, 8), (2, 4)))
    up_proj = bell_draw(key_list[5], (EXPERTS, D, F), D ** -0.5, 0.125, ((0, 8), (2, 4)))
    down_proj = bell_draw(key_list[6], (EXPERTS, F, D), F ** -0.5, 0.1875, ((0, 8), (1, 4)))
    out_proj = bell_draw(key_list[7], (D, SCAN_CHANNELS), SCAN_CHANNELS ** -0.5, 0.1875, ((1, 4),))
    conv_input = bell_draw(key_list[8], (STEP_COUNT, SCAN_CHANNELS), 1.0, 6.0, ((0, 8), (1, 4)))
    gate_branch = bell_draw(key_list[9], (STEP_COUNT, SCAN_CHANNELS), 1.0, 6.0, ((0, 8), (1, 4)))
    conv_taps = bell_draw(key_list[10], (CONV_W, SCAN_CHANNELS), 0.5, 3.0, ((1, 4),))
    recur_map = bell_draw(key_list[11], (2, SCAN_CHANNELS // HW, HW, HW), HW ** -0.5, 0.75, ((1, 4),))
    input_map = bell_draw(key_list[12], (2, SCAN_CHANNELS // HW, HW, HW), HW ** -0.5, 0.75, ((1, 4),))
    decay_param = draw_decay_param(jax.random.fold_in(key_list[15], 71), 0)
    decay_shift = draw_decay_shift(jax.random.fold_in(key_list[15], 71), 0)
    return {"cotangent": cotangent, "saved_input": saved_input, "routes": routes, "route_weight": route_weight, "gate_proj": gate_proj, "up_proj": up_proj, "down_proj": down_proj, "out_proj": out_proj, "conv_input": conv_input, "gate_branch": gate_branch, "conv_taps": conv_taps, "recur_map": recur_map, "input_map": input_map, "decay_param": decay_param, "decay_shift": decay_shift}


EPS = 1e-06
DECAY_SCALE = 8.0

def block_matrix(maps):
    heads = maps.shape[0]
    eye = jnp.eye(heads, dtype=jnp.float32)
    full = jnp.einsum('hij,hg->higj', maps.astype(jnp.float32), eye)
    return full.reshape(heads * maps.shape[1], heads * maps.shape[2])

def gate_terms(conv_out, recur_map, input_map, decay_param, decay_shift):
    recur = jax.nn.sigmoid(jnp.dot(conv_out, block_matrix(recur_map), precision=lax.Precision.HIGHEST))
    inputs = jax.nn.sigmoid(jnp.dot(conv_out, block_matrix(input_map), precision=lax.Precision.HIGHEST))
    log_decay = -DECAY_SCALE * recur * jax.nn.softplus(-decay_param)[None, :] + decay_shift
    decay = jnp.exp(log_decay)
    drive = jnp.sqrt(-jnp.expm1(2.0 * log_decay)) * (inputs * conv_out)
    return (decay, drive)

def link(earlier, later):
    return (earlier[0] * later[0], later[0] * earlier[1] + later[1])

def reference(cotangent, saved_input, routes, route_weight, gate_proj, up_proj, down_proj, out_proj, conv_input, gate_branch, conv_taps, recur_map, input_map, decay_param, decay_shift):
    inputs32 = saved_input.astype(jnp.float32)
    inv_rms = lax.rsqrt(lax.optimization_barrier(jnp.mean(inputs32 * inputs32, axis=1, keepdims=True)) + EPS)
    normed = inputs32 * inv_rms
    expert_input = normed.astype(jnp.bfloat16)
    scaled = (route_weight[:, :, None] * cotangent.astype(jnp.float32)[:, None, :]).astype(jnp.bfloat16)
    scaled = scaled.reshape(STEP_COUNT * TOP_K, D)
    flat_expert = routes.reshape(-1).astype(jnp.int32)
    order = jnp.argsort(flat_expert, stable=True).astype(jnp.int32)
    counts = lax.optimization_barrier(jnp.sum((flat_expert[:, None] == jnp.arange(EXPERTS, dtype=jnp.int32)[None, :]).astype(jnp.int32), axis=0)).astype(jnp.int32)
    starts = (jnp.cumsum(counts) - counts).astype(jnp.int32)
    most_rows = N_SP * CAP
    padded_order = jnp.concatenate([order, jnp.zeros((most_rows,), jnp.int32)])
    block = F // N_TP

    def one_expert(expert):
        picks = lax.dynamic_slice_in_dim(padded_order, starts[expert], most_rows)
        live = jnp.arange(most_rows, dtype=jnp.int32) < counts[expert]
        rows_input = jnp.where(live[:, None], expert_input[picks // TOP_K], 0.0).astype(jnp.bfloat16)
        rows_scaled = jnp.where(live[:, None], scaled[picks], 0.0).astype(jnp.bfloat16)
        w_gate = gate_proj[expert]
        w_up = up_proj[expert]
        w_down = down_proj[expert]
        gate_pre = jnp.dot(rows_input, w_gate, preferred_element_type=jnp.float32)
        up_pre = jnp.dot(rows_input, w_up, preferred_element_type=jnp.float32)
        gate_sig = jax.nn.sigmoid(gate_pre)
        gate_act = gate_pre * gate_sig
        hidden = (gate_act * up_pre).astype(jnp.bfloat16)
        hidden_grad = jnp.dot(rows_scaled, w_down.T, preferred_element_type=jnp.float32)
        gate_grad = (hidden_grad * up_pre * gate_sig * (1.0 + gate_pre * (1.0 - gate_sig))).astype(jnp.bfloat16)
        up_grad = (hidden_grad * gate_act).astype(jnp.bfloat16)
        grad_down = jnp.dot(hidden.T, rows_scaled, preferred_element_type=jnp.float32)
        grad_gate = jnp.dot(rows_input.T, gate_grad, preferred_element_type=jnp.float32)
        grad_up = jnp.dot(rows_input.T, up_grad, preferred_element_type=jnp.float32)
        pieces = jnp.zeros((most_rows, D), jnp.float32)
        for step_number in range(N_TP):
            low = step_number * block
            piece = jnp.dot(gate_grad[:, low:low + block], w_gate[:, low:low + block].T, preferred_element_type=jnp.float32)
            piece = piece + jnp.dot(up_grad[:, low:low + block], w_up[:, low:low + block].T, preferred_element_type=jnp.float32)
            rounded = lax.optimization_barrier(piece.astype(jnp.bfloat16))
            pieces = pieces + rounded.astype(jnp.float32)
        route_rows = pieces.astype(jnp.bfloat16)
        target = jnp.where(live, picks, STEP_COUNT * TOP_K).astype(jnp.int32)
        return (grad_gate, grad_up, grad_down, route_rows, target)
    grad_gate_proj, grad_up_proj, grad_down_proj, route_rows, targets = lax.map(one_expert, jnp.arange(EXPERTS, dtype=jnp.int32))
    assigned = jnp.zeros((STEP_COUNT * TOP_K + 1, D), jnp.bfloat16).at[targets.reshape(-1)].set(route_rows.reshape(-1, D))
    normed_grad = lax.optimization_barrier(jnp.sum(assigned[:STEP_COUNT * TOP_K].reshape(STEP_COUNT, TOP_K, D).astype(jnp.float32), axis=1))
    mixed_grad = cotangent.astype(jnp.float32) + inv_rms * (normed_grad - normed * lax.optimization_barrier(jnp.mean(normed_grad * normed, axis=1, keepdims=True)))
    mixed_grad_b = mixed_grad.astype(jnp.bfloat16)
    taps32 = conv_taps.astype(jnp.float32)

    def mixer(conv_in, branch):
        padded = jnp.pad(conv_in, ((2, 1), (0, 0)))
        conv_out = jnp.zeros((STEP_COUNT, SCAN_CHANNELS), jnp.float32)
        for offset in range(CONV_W):
            conv_out = conv_out + padded[offset:offset + STEP_COUNT] * taps32[offset]
        states = jnp.zeros((STEP_COUNT, SCAN_CHANNELS), jnp.float32)
        for direction in range(2):
            decay, drive = gate_terms(conv_out, recur_map[direction], input_map[direction], decay_param[direction], decay_shift[direction])
            states = states + lax.associative_scan(link, (decay, drive), axis=0, reverse=direction == 1)[1]
        return jax.nn.gelu(branch) * states
    value, pull = jax.vjp(mixer, conv_input.astype(jnp.float32), gate_branch.astype(jnp.float32))
    mixed_out = value.astype(jnp.bfloat16)
    grad_out_proj = lax.dot_general(mixed_grad_b, mixed_out, (((0,), (0,)), ((), ())), preferred_element_type=jnp.float32)
    out_grad = jnp.dot(mixed_grad_b, out_proj, preferred_element_type=jnp.float32)
    conv_grad, branch_grad = pull(out_grad)
    return (grad_gate_proj, grad_up_proj, grad_down_proj, grad_out_proj, conv_grad.astype(jnp.bfloat16), branch_grad.astype(jnp.bfloat16))
```

```python
import functools
import jax
import jax.numpy as jnp
from jax import lax
from jax.experimental import pallas as pl
from jax.experimental.pallas import tpu as pltpu
from jax.sharding import PartitionSpec as P

EPS = 1e-06
DECAY_SCALE = 8.0
ROW_TILE = 16
GELU_K = 0.7978845608028654
GELU_C = 0.044715
VM = pl.BlockSpec(memory_space=pltpu.VMEM)
BF = jnp.bfloat16
F32 = jnp.float32


def local_call(kernel, args, outs, cost=10_000_000):
    return pl.pallas_call(
        kernel,
        out_shape=outs,
        in_specs=[VM] * len(args),
        out_specs=jax.tree.map(lambda _: VM, outs),
        compiler_params=pltpu.CompilerParams(vmem_limit_bytes=56 * 2**20),
        cost_estimate=pl.CostEstimate(flops=cost, bytes_accessed=4_000_000, transcendentals=0),
    )(*args)


def prepare_kernel(slots, cot_ref, x_ref, routes_ref, weight_ref, sends_ref, sendi_ref, pick_ref):
    length, width = cot_ref.shape
    experts = sends_ref.shape[0]
    fourth = sends_ref.shape[2]
    tp = lax.axis_index("tp")
    cols = pl.ds(pl.multiple_of(tp * fourth, 128), fourth)
    x = x_ref[...].astype(F32)
    inv = lax.rsqrt(jnp.mean(x * x, axis=1, keepdims=True) + EPS)
    mine = (x_ref[:, cols].astype(F32) * inv).astype(BF)
    routes = routes_ref[...]
    weight = weight_ref[...]
    which = lax.broadcasted_iota(jnp.int32, (experts, length), 0)
    first = which == routes[0:1]
    second = which == routes[1:2]
    named = (first | second).astype(F32).astype(BF)
    earlier = lax.broadcasted_iota(jnp.int32, (length, length), 0) < lax.broadcasted_iota(
        jnp.int32, (length, length), 1
    )
    rank = jnp.dot(named, earlier.astype(F32).astype(BF), preferred_element_type=F32)
    place = which * slots + rank.astype(jnp.int32)
    target0 = jnp.sum(jnp.where(first, place, 0).astype(F32), axis=0, keepdims=True).astype(jnp.int32)
    target1 = jnp.sum(jnp.where(second, place, 0).astype(F32), axis=0, keepdims=True).astype(jnp.int32)
    slot = lax.broadcasted_iota(jnp.int32, (experts * slots, length), 0)
    hit0 = slot == target0
    hit1 = slot == target1
    pick = (hit0 | hit1).astype(F32).astype(BF)
    pick_ref[...] = pick
    share = jnp.where(hit0, weight[0:1], 0.0) + jnp.where(hit1, weight[1:2], 0.0)
    share = jnp.sum(share, axis=1, keepdims=True)
    got = jnp.dot(pick, mine, preferred_element_type=F32).astype(BF)
    sendi_ref[...] = got.reshape(experts, slots, fourth)
    cot = jnp.dot(pick, cot_ref[:, cols], preferred_element_type=F32)
    sends_ref[...] = (cot * share).astype(BF).reshape(experts, slots, fourth)


def neighbours():
    tp = lax.axis_index("tp")
    side = tp // 2
    core = tp % 2
    return tp, side * 2 + (1 - core), (1 - side) * 2 + core, (1 - side) * 2 + (1 - core)


def greet(n, with_sp=True, with_tp=True):
    sp = lax.axis_index("sp")
    tp, partner, across, _ = neighbours()
    barrier = pltpu.get_barrier_semaphore()
    count = 0
    if with_sp:
        for d in range(1, n):
            pl.semaphore_signal(
                barrier, inc=1, device_id=((sp + d) % n, tp), device_id_type=pl.DeviceIdType.MESH
            )
        count += n - 1
    if with_tp:
        for other in (partner, across):
            pl.semaphore_signal(
                barrier, inc=1, device_id=(sp, other), device_id_type=pl.DeviceIdType.MESH
            )
        count += 2
    pl.semaphore_wait(barrier, count)


def remote(src, dst, sems, index, device):
    return pltpu.make_async_remote_copy(
        src_ref=src,
        dst_ref=dst,
        send_sem=sems.at[(0,) + index],
        recv_sem=sems.at[(1,) + index],
        device_id=device,
        device_id_type=pl.DeviceIdType.MESH,
    )


def dispatch_kernel(n, sends_ref, sendi_ref, outs_ref, outi_ref, hop, pair, cross, fwd, own):
    fourth = sends_ref.shape[2]
    sp = lax.axis_index("sp")
    tp, partner, across, _ = neighbours()

    def cols(q):
        return pl.ds(pl.multiple_of(q * fourth, 128), fourth)

    mine, theirs = cols(tp), cols(across)
    arrays = ((sends_ref, outs_ref), (sendi_ref, outi_ref))
    greet(n)
    hops = {}
    pending = []
    for a, (src, dst) in enumerate(arrays):
        local = pltpu.make_async_copy(src.at[sp], dst.at[sp, :, mine], own.at[a])
        local.start()
        hops[a, 0] = local
    for d in range(1, n):
        peer = (sp + d) % n
        for a, (src, dst) in enumerate(arrays):
            copy = remote(src.at[peer], dst.at[sp, :, mine], hop, (a, d), (peer, tp))
            copy.start()
            hops[a, d] = copy

    def step_in(a, d):
        dst = arrays[a][1]
        source = (sp + n - d) % n
        if d == 0:
            hops[a, d].wait()
        else:
            hops[a, d].wait_recv()
        block = dst.at[source, :, mine]
        over = remote(block, block, cross, (a, d), (sp, across))
        over.start()
        near = remote(block, block, pair, (a, d), (sp, partner))
        near.start()
        pending.append(near)
        return over

    def step_on(a, d, over):
        dst = arrays[a][1]
        source = (sp + n - d) % n
        over.wait_recv()
        block = dst.at[source, :, theirs]
        copy = remote(block, block, fwd, (a, d), (sp, partner))
        copy.start()
        pending.append(copy)

    order = [(a, d) for d in range(n) for a in range(2)]
    overs = []
    lag = 2
    for i, (a, d) in enumerate(order):
        overs.append(step_in(a, d))
        if i >= lag:
            step_on(*order[i - lag], overs[i - lag])
    for i in range(max(len(order) - lag, 0), len(order)):
        step_on(*order[i], overs[i])
    for copy in pending:
        copy.wait()
    for over in overs:
        over.wait_send()
    for d in range(1, n):
        for a in range(2):
            hops[a, d].wait_send()


def dispatch(sends, sendi, n, n_tp):
    experts, slots, fourth = sends.shape
    full = jax.ShapeDtypeStruct((experts, slots, fourth * n_tp), BF)
    dma = pltpu.SemaphoreType.DMA
    return pl.pallas_call(
        functools.partial(dispatch_kernel, n),
        out_shape=(full, full),
        in_specs=[VM, VM],
        out_specs=(VM, VM),
        scratch_shapes=[dma((2, 2, n))] * 4 + [dma((2,))],
        compiler_params=pltpu.CompilerParams(
            collective_id=1, has_side_effects=True, vmem_limit_bytes=40 * 2**20
        ),
        cost_estimate=pl.CostEstimate(flops=0, bytes_accessed=100_000_000, transcendentals=0),
    )(sends, sendi)


def return_kernel(
    n, part_ref, pick_ref, out_ref, got1, got2, mid, fin, back, s_pair, s_cross, s_hop, s_tail
):
    fourth = got2.shape[2]
    slots = got2.shape[1]
    sp = lax.axis_index("sp")
    tp, partner, across, diagonal = neighbours()

    def cols(q):
        return pl.ds(pl.multiple_of(q * fourth, 128), fourth)

    greet(n)
    order = list(range(1, n)) + [0]
    pairs, crosses, hops = {}, {}, {}
    for d in order:
        j = (sp + d) % n
        for a, q in enumerate((diagonal, partner)):
            copy = remote(
                part_ref.at[j, :, cols(q)], got1.at[a, j], s_pair, (a, d), (sp, partner)
            )
            copy.start()
            pairs[a, d] = copy

    def stage_b(d):
        j = (sp + d) % n
        pairs[0, d].wait_recv()
        total = part_ref[j, :, cols(across)].astype(F32) + got1[0, j].astype(F32)
        mid[j] = total.astype(BF)
        copy = remote(mid.at[j], got2.at[j], s_cross, (d,), (sp, across))
        copy.start()
        crosses[d] = copy

    def stage_c(d):
        j = (sp + d) % n
        pairs[1, d].wait_recv()
        crosses[d].wait_recv()
        total = part_ref[j, :, cols(tp)].astype(F32) + got1[1, j].astype(F32)
        total = (total + got2[j].astype(F32)).astype(BF)
        if d == 0:
            back[sp] = total
        else:
            fin[j] = total
            copy = remote(fin.at[j], back.at[sp], s_hop, (d,), (j, tp))
            copy.start()
            hops[d] = copy

    lag = 2
    for i, d in enumerate(order):
        stage_b(d)
        if i >= lag:
            stage_c(order[i - lag])
    for d in order[max(n - lag, 0):]:
        stage_c(d)
    for d in range(1, n):
        hops[d].wait_recv()
    rows = back[...].reshape(n * slots, fourth)
    grad = lax.dot_general(
        pick_ref[...], rows, (((0,), (0,)), ((), ())), preferred_element_type=F32
    )
    out_ref[:, cols(tp)] = grad.astype(BF)
    own = out_ref.at[:, cols(tp)]
    over = remote(own, own, s_tail, (0,), (sp, across))
    near = remote(own, own, s_tail, (1,), (sp, partner))
    over.start()
    near.start()
    over.wait_recv()
    other = out_ref.at[:, cols(across)]
    last = remote(other, other, s_tail, (2,), (sp, partner))
    last.start()
    for d in range(n):
        for a in range(2):
            pairs[a, d].wait_send()
        crosses[d].wait_send()
        if d:
            hops[d].wait_send()
    near.wait()
    over.wait_send()
    last.wait()


def send_back(part, pick, n, n_tp):
    _, slots, width = part.shape
    fourth = width // n_tp
    dma = pltpu.SemaphoreType.DMA
    block = (n, slots, fourth)
    return pl.pallas_call(
        functools.partial(return_kernel, n),
        out_shape=jax.ShapeDtypeStruct((pick.shape[1], width), BF),
        in_specs=[VM, VM],
        out_specs=VM,
        scratch_shapes=[pltpu.VMEM((2,) + block, BF)]
        + [pltpu.VMEM(block, BF)] * 4
        + [dma((2, 2, n)), dma((2, n)), dma((2, n)), dma((2, 3))],
        compiler_params=pltpu.CompilerParams(
            collective_id=2, has_side_effects=True, vmem_limit_bytes=40 * 2**20
        ),
        cost_estimate=pl.CostEstimate(flops=0, bytes_accessed=100_000_000, transcendentals=0),
    )(part, pick)


def exchange_kernel(n, same, src_ref, dst_ref, sems, own):
    sp = lax.axis_index("sp")
    tp = lax.axis_index("tp")

    def piece(i):
        return src_ref if same else src_ref.at[i]

    greet(n, with_tp=False)
    local = pltpu.make_async_copy(piece(sp), dst_ref.at[sp], own.at[0])
    local.start()
    copies = []
    for d in range(1, n):
        peer = (sp + d) % n
        copy = remote(piece(peer), dst_ref.at[sp], sems, (d,), (peer, tp))
        copy.start()
        copies.append(copy)
    local.wait()
    for copy in copies:
        copy.wait()


def exchange(x, n, same, cid):
    shape = (n,) + x.shape if same else x.shape
    dma = pltpu.SemaphoreType.DMA
    return pl.pallas_call(
        functools.partial(exchange_kernel, n, same),
        out_shape=jax.ShapeDtypeStruct(shape, x.dtype),
        in_specs=[VM],
        out_specs=VM,
        scratch_shapes=[dma((2, n)), dma((1,))],
        compiler_params=pltpu.CompilerParams(
            collective_id=cid, has_side_effects=True, vmem_limit_bytes=24 * 2**20
        ),
        cost_estimate=pl.CostEstimate(flops=0, bytes_accessed=20_000_000, transcendentals=0),
    )(x)


def split_dot(x, w, dims):
    high = x.astype(BF)
    rest = x - high.astype(F32)
    middle = rest.astype(BF)
    low = (rest - middle.astype(F32)).astype(BF)
    total = lax.dot_general(low, w, dims, preferred_element_type=F32)
    total = total + lax.dot_general(middle, w, dims, preferred_element_type=F32)
    return total + lax.dot_general(high, w, dims, preferred_element_type=F32)


def minus_expm1(y):
    series = 1.0 + y * (1.0 / 8.0)
    for k in (7.0, 6.0, 5.0, 4.0, 3.0, 2.0):
        series = 1.0 + y * (1.0 / k) * series
    return jnp.where(y > -0.25, -y * series, 1.0 - jnp.exp(y))


def shifted(x, by, edge):
    length = x.shape[0]
    row = lax.broadcasted_iota(jnp.int32, x.shape, 0)
    moved = pltpu.roll(x, by % length, 0)
    return jnp.where(row == (0 if by > 0 else length - 1), edge, moved)


def run_scans(length, jobs):
    width = jobs[0][1].shape[1]
    groups = length // 8

    def body(g, carry):
        out = []
        for (reverse, a_ref, b_ref, to_ref), state in zip(jobs, carry):
            base = pl.multiple_of((groups - 1 - g if reverse else g) * 8, 8)
            a = a_ref[pl.ds(base, 8), :]
            b = None if b_ref is None else b_ref[pl.ds(base, 8), :]
            rows = [None] * 8
            for k in reversed(range(8)) if reverse else range(8):
                state = a[k : k + 1] * state
                if b is not None:
                    state = state + b[k : k + 1]
                rows[k] = state
            to_ref[pl.ds(base, 8), :] = jnp.concatenate(rows, axis=0)
            out.append(state)
        return tuple(out)

    start = tuple(
        jnp.full((1, width), 1.0 if b_ref is None else 0.0, F32) for _, _, b_ref, _ in jobs
    )
    return lax.fori_loop(0, groups, body, start)


def pre_kernel(
    x_ref, low_ref, high_ref, taps_ref, maps_ref, plus_ref, shift_ref,
    conv_ref, gates_ref, decay_ref, root_ref, state_ref, cum_ref, after_ref, tot_ref, drive_ref,
):
    length, width = x_ref.shape
    taps = taps_ref[...].astype(F32)
    low = low_ref[...].astype(F32)
    high = high_ref[...].astype(F32)
    x = x_ref[...].astype(F32)
    back1 = shifted(x, 1, low[1:2])
    back2 = shifted(back1, 1, low[0:1])
    conv = back2 * taps[0:1] + back1 * taps[1:2] + x * taps[2:3]
    conv = conv + shifted(x, -1, high[0:1]) * taps[3:4]
    conv_ref[...] = conv
    gates = jax.nn.sigmoid(split_dot(conv, maps_ref[...], (((1,), (0,)), ((), ()))))
    gates_ref[...] = gates
    for d in range(2):
        recur = gates[:, 2 * d * width : (2 * d + 1) * width]
        inputs = gates[:, (2 * d + 1) * width : (2 * d + 2) * width]
        log_decay = -DECAY_SCALE * recur * plus_ref[d : d + 1, :] + shift_ref[d]
        root = jnp.sqrt(minus_expm1(2.0 * log_decay))
        decay_ref[d] = jnp.exp(log_decay)
        root_ref[d] = root
        drive_ref[d] = root * (inputs * conv)
    a_f, a_b = decay_ref.at[0], decay_ref.at[1]
    ends = run_scans(
        length,
        (
            (False, a_f, drive_ref.at[0], state_ref.at[0]),
            (True, a_b, drive_ref.at[1], state_ref.at[1]),
            (False, a_f, None, cum_ref.at[0]),
            (True, a_b, None, cum_ref.at[1]),
            (True, a_f, None, after_ref.at[0]),
            (False, a_b, None, after_ref.at[1]),
        ),
    )
    tot_ref[0:1, :] = ends[2]
    tot_ref[1:2, :] = ends[0]
    tot_ref[2:3, :] = ends[3]
    tot_ref[3:4, :] = ends[1]
    tot_ref[4:8, :] = jnp.zeros((4, width), F32)


def gelu_parts(x):
    t = jnp.tanh(GELU_K * (x + GELU_C * x * x * x))
    value = 0.5 * x * (1.0 + t)
    slope = 0.5 * (1.0 + t) + 0.5 * x * (1.0 - t * t) * GELU_K * (1.0 + 3.0 * GELU_C * x * x)
    return value, slope


def middle_kernel(
    ng_ref, cot_ref, x_ref, proj_ref, branch_ref, decay_ref, tot_ref,
    mixed_ref, out_grad_ref, carried_ref, after_ref, tot2_ref, drive_ref,
):
    length = ng_ref.shape[0]
    x = x_ref[...].astype(F32)
    inv = lax.rsqrt(jnp.mean(x * x, axis=1, keepdims=True) + EPS)
    normed = x * inv
    ng = ng_ref[...].astype(F32)
    dot = jnp.mean(ng * normed, axis=1, keepdims=True)
    mixed = (cot_ref[...].astype(F32) + inv * (ng - normed * dot)).astype(BF)
    mixed_ref[...] = mixed
    out_grad = jnp.dot(mixed, proj_ref[...], preferred_element_type=F32)
    out_grad_ref[...] = out_grad
    value, _ = gelu_parts(branch_ref[...].astype(F32))
    carried = out_grad * value
    carried_ref[...] = carried
    drive_ref[...] = decay_ref[...] * carried[None]
    ends = run_scans(
        length,
        (
            (True, decay_ref.at[0], drive_ref.at[0], after_ref.at[0]),
            (False, decay_ref.at[1], drive_ref.at[1], after_ref.at[1]),
        ),
    )
    tot2_ref[0:4, :] = tot_ref[0:4, :]
    tot2_ref[4:5, :] = ends[1]
    tot2_ref[5:6, :] = ends[0]
    tot2_ref[6:8, :] = jnp.zeros((2, tot_ref.shape[1]), F32)


def last_kernel(
    n, all_ref, conv_ref, gates_ref, decay_ref, root_ref, state_ref, cum_ref, ones_ref,
    after_ref, carried_ref, out_grad_ref, branch_ref, maps_ref, plus_ref,
    conv_grad_ref, branch_grad_ref, mixed_out_ref, packed_ref,
):
    length, width = conv_ref.shape
    sp = lax.axis_index("sp")
    zero = jnp.zeros((1, width), F32)

    def lower(k, carry):
        t = all_ref[k]
        return (t[0:1] * carry[0] + t[1:2], t[2:3] * carry[1] + t[4:5])

    def upper(i, carry):
        t = all_ref[n - 1 - i]
        return (t[2:3] * carry[0] + t[3:4], t[0:1] * carry[1] + t[5:6])

    in_f, in_ab = lax.fori_loop(0, sp, lower, (zero, zero))
    in_b, in_af = lax.fori_loop(0, n - 1 - sp, upper, (zero, zero))
    state_f = state_ref[0] + cum_ref[0] * in_f
    state_b = state_ref[1] + cum_ref[1] * in_b
    after_f = after_ref[0] + ones_ref[0] * in_af
    after_b = after_ref[1] + ones_ref[1] * in_ab
    carried = carried_ref[...]
    adjoint = (carried + shifted(after_f, -1, in_af), carried + shifted(after_b, 1, in_ab))
    beside = (shifted(state_f, 1, in_f), shifted(state_b, -1, in_b))
    conv = conv_ref[...]
    total = jnp.zeros((length, width), F32)
    for d in range(2):
        recur = gates_ref[:, 2 * d * width : (2 * d + 1) * width]
        inputs = gates_ref[:, (2 * d + 1) * width : (2 * d + 2) * width]
        decay = decay_ref[d]
        root = root_ref[d]
        g = adjoint[d]
        total = total + g * root * inputs
        g_log = g * beside[d] * decay - g * inputs * conv * (decay * decay) / root
        g_recur = g_log * (-DECAY_SCALE * plus_ref[d : d + 1, :])
        packed_ref[:, 2 * d * width : (2 * d + 1) * width] = g_recur * recur * (1.0 - recur)
        packed_ref[:, (2 * d + 1) * width : (2 * d + 2) * width] = (
            g * root * conv * inputs * (1.0 - inputs)
        )
    total = total + split_dot(packed_ref[...], maps_ref[...], (((1,), (1,)), ((), ())))
    conv_grad_ref[...] = total.astype(BF)
    value, slope = gelu_parts(branch_ref[...].astype(F32))
    states = state_f + state_b
    mixed_out_ref[...] = (value * states).astype(BF)
    branch_grad_ref[...] = (out_grad_ref[...] * states * slope).astype(BF)


def block_matrix(maps):
    heads = maps.shape[0]
    eye = jnp.eye(heads, dtype=maps.dtype)
    full = maps[:, :, None, :] * eye[:, None, :, None]
    return full.reshape(heads * maps.shape[1], heads * maps.shape[2])


def edge_rows(block, n, width):
    forward = [(i, i + 1) for i in range(n - 1)]
    backward = [(i + 1, i) for i in range(n - 1)]
    low = lax.ppermute(block[block.shape[0] - width :], "sp", forward)
    high = lax.ppermute(block[:width], "sp", backward)
    return low, high


def shards(
    cotangent,
    saved_input,
    routes,
    route_weight,
    gate_proj,
    up_proj,
    down_proj,
    out_proj,
    conv_input,
    gate_branch,
    conv_taps,
    recur_map,
    input_map,
    decay_param,
    decay_shift,
):
    length, width = cotangent.shape
    n = lax.axis_size("sp")
    n_tp = lax.axis_size("tp")
    experts = n * gate_proj.shape[0]
    slots = 4 * length // n
    slots = (slots + ROW_TILE - 1) // ROW_TILE * ROW_TILE
    fourth = width // n_tp
    channels = conv_input.shape[1]
    sds = jax.ShapeDtypeStruct

    low, high = edge_rows(conv_input, n, 2)
    sends, sendi, pick = local_call(
        functools.partial(prepare_kernel, slots),
        (cotangent, saved_input, routes.T, route_weight.T),
        (
            sds((experts, slots, fourth), BF),
            sds((experts, slots, fourth), BF),
            sds((experts * slots, length), BF),
        ),
    )
    got_scaled, got_input = dispatch(sends, sendi, n, n_tp)
    rows_scaled = got_scaled.reshape(experts * slots, width)
    rows_input = got_input.reshape(experts * slots, width)
    w_gate = gate_proj[0]
    w_up = up_proj[0]
    w_down = down_proj[0]
    gate_pre = jnp.dot(rows_input, w_gate, preferred_element_type=F32)
    up_pre = jnp.dot(rows_input, w_up, preferred_element_type=F32)
    gate_sig = jax.nn.sigmoid(gate_pre)
    gate_act = gate_pre * gate_sig
    hidden = (gate_act * up_pre).astype(BF)
    hidden_grad = lax.dot_general(
        rows_scaled, w_down, (((1,), (1,)), ((), ())), preferred_element_type=F32
    )
    gate_grad = (hidden_grad * up_pre * gate_sig * (1.0 + gate_pre * (1.0 - gate_sig))).astype(BF)
    up_grad = (hidden_grad * gate_act).astype(BF)
    partial_rows = lax.dot_general(
        gate_grad, w_gate, (((1,), (1,)), ((), ())), preferred_element_type=F32
    )
    partial_rows = partial_rows + lax.dot_general(
        up_grad, w_up, (((1,), (1,)), ((), ())), preferred_element_type=F32
    )
    part = partial_rows.astype(BF).reshape(experts, slots, width)
    normed_grad = send_back(part, pick, n, n_tp)
    rows0 = (((0,), (0,)), ((), ()))
    grad_down = lax.dot_general(hidden, rows_scaled, rows0, preferred_element_type=F32)
    grad_gate = lax.dot_general(rows_input, gate_grad, rows0, preferred_element_type=F32)
    grad_up = lax.dot_general(rows_input, up_grad, rows0, preferred_element_type=F32)

    maps = jnp.concatenate(
        [block_matrix(m[d]) for d in range(2) for m in (recur_map, input_map)], axis=1
    )
    plus = jax.nn.softplus(-decay_param)
    one = sds((length, channels), F32)
    two = sds((2, length, channels), F32)
    eight = sds((8, channels), F32)
    conv, gates, decay, root, state, cum, ones, tot, _ = local_call(
        pre_kernel,
        (conv_input, low, high, conv_taps, maps, plus, decay_shift),
        (one, sds((length, 4 * channels), F32), two, two, two, two, two, eight, two),
    )
    mixed_grad_b, out_grad, carried, after, tot2, _ = local_call(
        middle_kernel,
        (normed_grad, cotangent, saved_input, out_proj, gate_branch, decay, tot),
        (sds((length, width), BF), one, one, two, eight, two),
    )
    everyone = exchange(tot2, n, True, 3)
    conv_grad, branch_grad, mixed_out, _ = local_call(
        functools.partial(last_kernel, n),
        (
            everyone, conv, gates, decay, root, state, cum, ones, after, carried, out_grad,
            gate_branch, maps, plus,
        ),
        (
            sds((length, channels), BF),
            sds((length, channels), BF),
            sds((length, channels), BF),
            sds((length, 4 * channels), F32),
        ),
    )
    grad_low, grad_high = edge_rows(conv_grad, n, 2)
    grad_part = lax.dot_general(mixed_grad_b, mixed_out, rows0, preferred_element_type=F32)
    pieces = exchange(grad_part.astype(BF).reshape(n, width // n, channels), n, False, 4)
    grad_out = jnp.sum(pieces.astype(F32), axis=0)
    taps32 = conv_taps.astype(F32)
    grad_pad = jnp.concatenate([grad_low, conv_grad, grad_high], axis=0).astype(F32)
    input_grad = jnp.zeros((length, channels), F32)
    for offset in range(taps32.shape[0]):
        input_grad = input_grad + grad_pad[4 - offset : 4 - offset + length] * taps32[offset]
    return (
        grad_gate[None],
        grad_up[None],
        grad_down[None],
        grad_out,
        input_grad.astype(BF),
        branch_grad,
    )


def solution(mesh):
    in_specs = (
        P("sp", None),
        P("sp", None),
        P("sp", None),
        P("sp", None),
        P("sp", None, "tp"),
        P("sp", None, "tp"),
        P("sp", "tp", None),
        P(None, "tp"),
        P("sp", "tp"),
        P("sp", "tp"),
        P(None, "tp"),
        P(None, "tp", None, None),
        P(None, "tp", None, None),
        P(None, "tp"),
        P(None, "sp", "tp"),
    )
    out_specs = (
        P("sp", None, "tp"),
        P("sp", None, "tp"),
        P("sp", "tp", None),
        P("sp", "tp"),
        P("sp", "tp"),
        P("sp", "tp"),
    )
    return jax.shard_map(shards, mesh=mesh, in_specs=in_specs, out_specs=out_specs, check_vma=False)
```

```python
import functools
import jax
import jax.numpy as jnp
from jax import lax
from jax.experimental import pallas as pl
from jax.experimental.pallas import tpu as pltpu
from jax.sharding import PartitionSpec as P

EPS = 1e-06
DECAY_SCALE = 8.0
ROW_TILE = 16
GELU_K = 0.7978845608028654
GELU_C = 0.044715
VM = pl.BlockSpec(memory_space=pltpu.VMEM)
BF = jnp.bfloat16
F32 = jnp.float32


def local_call(kernel, args, outs, cost=10_000_000):
    return pl.pallas_call(
        kernel,
        out_shape=outs,
        in_specs=[VM] * len(args),
        out_specs=jax.tree.map(lambda _: VM, outs),
        compiler_params=pltpu.CompilerParams(vmem_limit_bytes=56 * 2**20),
        cost_estimate=pl.CostEstimate(flops=cost, bytes_accessed=4_000_000, transcendentals=0),
    )(*args)


def prepare_kernel(slots, cot_ref, x_ref, routes_ref, weight_ref, sends_ref, sendi_ref, pick_ref):
    length, width = cot_ref.shape
    experts = sends_ref.shape[0]
    fourth = sends_ref.shape[2]
    tp = lax.axis_index("tp")
    cols = pl.ds(pl.multiple_of(tp * fourth, 128), fourth)
    x = x_ref[...].astype(F32)
    inv = lax.rsqrt(jnp.mean(x * x, axis=1, keepdims=True) + EPS)
    mine = (x_ref[:, cols].astype(F32) * inv).astype(BF)
    routes = routes_ref[...]
    weight = weight_ref[...]
    which = lax.broadcasted_iota(jnp.int32, (experts, length), 0)
    first = which == routes[0:1]
    second = which == routes[1:2]
    named = (first | second).astype(F32).astype(BF)
    earlier = lax.broadcasted_iota(jnp.int32, (length, length), 0) < lax.broadcasted_iota(
        jnp.int32, (length, length), 1
    )
    rank = jnp.dot(named, earlier.astype(F32).astype(BF), preferred_element_type=F32)
    place = which * slots + rank.astype(jnp.int32)
    target0 = jnp.sum(jnp.where(first, place, 0).astype(F32), axis=0, keepdims=True).astype(jnp.int32)
    target1 = jnp.sum(jnp.where(second, place, 0).astype(F32), axis=0, keepdims=True).astype(jnp.int32)
    slot = lax.broadcasted_iota(jnp.int32, (experts * slots, length), 0)
    hit0 = slot == target0
    hit1 = slot == target1
    pick = (hit0 | hit1).astype(F32).astype(BF)
    pick_ref[...] = pick
    share = jnp.where(hit0, weight[0:1], 0.0) + jnp.where(hit1, weight[1:2], 0.0)
    share = jnp.sum(share, axis=1, keepdims=True)
    got = jnp.dot(pick, mine, preferred_element_type=F32).astype(BF)
    sendi_ref[...] = got.reshape(experts, slots, fourth)
    cot = jnp.dot(pick, cot_ref[:, cols], preferred_element_type=F32)
    sends_ref[...] = (cot * share).astype(BF).reshape(experts, slots, fourth)


def neighbours():
    tp = lax.axis_index("tp")
    side = tp // 2
    core = tp % 2
    return tp, side * 2 + (1 - core), (1 - side) * 2 + core, (1 - side) * 2 + (1 - core)


def greet(n, with_sp=True, with_tp=True):
    sp = lax.axis_index("sp")
    tp, partner, across, _ = neighbours()
    barrier = pltpu.get_barrier_semaphore()
    count = 0
    if with_sp:
        for d in range(1, n):
            pl.semaphore_signal(
                barrier, inc=1, device_id=((sp + d) % n, tp), device_id_type=pl.DeviceIdType.MESH
            )
        count += n - 1
    if with_tp:
        for other in (partner, across):
            pl.semaphore_signal(
                barrier, inc=1, device_id=(sp, other), device_id_type=pl.DeviceIdType.MESH
            )
        count += 2
    pl.semaphore_wait(barrier, count)


def partner_at(sp, n, d):
    if n & (n - 1):
        return (sp + d) % n
    bit, peer = 1, sp
    while bit < n:
        if d & bit:
            peer = peer + bit * (1 - 2 * ((sp // bit) % 2))
        bit *= 2
    return peer


def source_at(sp, n, d):
    return (sp + n - d) % n if n & (n - 1) else partner_at(sp, n, d)


def edge_copies(n, x_ref, halo_ref, sems):
    sp = lax.axis_index("sp")
    tp = lax.axis_index("tp")
    length, tile = x_ref.shape[0], halo_ref.shape[1]
    copies = (
        remote(x_ref.at[pl.ds(length - tile, tile)], halo_ref.at[0], sems, (0,), ((sp + 1) % n, tp)),
        remote(x_ref.at[pl.ds(0, tile)], halo_ref.at[1], sems, (1,), ((sp + n - 1) % n, tp)),
    )
    for copy in copies:
        copy.start()
    return copies


def halo_edges(halo, n, width):
    sp = lax.axis_index("sp")
    zero = jnp.zeros((), halo.dtype)
    return (
        jnp.where(sp == 0, zero, halo[0, halo.shape[1] - width :]),
        jnp.where(sp == n - 1, zero, halo[1, :width]),
    )


def remote(src, dst, sems, index, device):
    return pltpu.make_async_remote_copy(
        src_ref=src,
        dst_ref=dst,
        send_sem=sems.at[(0,) + index],
        recv_sem=sems.at[(1,) + index],
        device_id=device,
        device_id_type=pl.DeviceIdType.MESH,
    )


def dispatch_kernel(
    n, sends_ref, sendi_ref, x_ref, outs_ref, outi_ref, halo_ref, hop, pair, cross, fwd, own, edge
):
    fourth = sends_ref.shape[2]
    sp = lax.axis_index("sp")
    tp, partner, across, _ = neighbours()

    def cols(q):
        return pl.ds(pl.multiple_of(q * fourth, 128), fourth)

    mine, theirs = cols(tp), cols(across)
    arrays = ((sends_ref, outs_ref), (sendi_ref, outi_ref))
    greet(n)
    hops = {}
    pending = list(edge_copies(n, x_ref, halo_ref, edge))
    away = [1] + [d for p in (0, 1) for d in range(n - 1, 1, -1) if d % 2 == p]
    for a, (src, dst) in enumerate(arrays):
        local = pltpu.make_async_copy(src.at[sp], dst.at[sp, :, mine], own.at[a])
        local.start()
        hops[a, 0] = local
    for d in away:
        peer = partner_at(sp, n, d)
        for a, (src, dst) in enumerate(arrays):
            copy = remote(src.at[peer], dst.at[sp, :, mine], hop, (a, d), (peer, tp))
            copy.start()
            hops[a, d] = copy

    def step_in(a, d):
        dst = arrays[a][1]
        source = source_at(sp, n, d)
        if d == 0:
            hops[a, d].wait()
        else:
            hops[a, d].wait_recv()
        block = dst.at[source, :, mine]
        over = remote(block, block, cross, (a, d), (sp, across))
        over.start()
        near = remote(block, block, pair, (a, d), (sp, partner))
        near.start()
        pending.append(near)
        return over

    def step_on(a, d, over):
        dst = arrays[a][1]
        source = source_at(sp, n, d)
        over.wait_recv()
        block = dst.at[source, :, theirs]
        copy = remote(block, block, fwd, (a, d), (sp, partner))
        copy.start()
        pending.append(copy)

    order = [(a, d) for d in [0] + away for a in range(2)]
    overs = []
    lag = 2
    for i, (a, d) in enumerate(order):
        overs.append(step_in(a, d))
        if i >= lag:
            step_on(*order[i - lag], overs[i - lag])
    for i in range(max(len(order) - lag, 0), len(order)):
        step_on(*order[i], overs[i])
    for copy in pending:
        copy.wait()
    for over in overs:
        over.wait_send()
    for d in range(1, n):
        for a in range(2):
            hops[a, d].wait_send()


def dispatch(sends, sendi, x, n, n_tp):
    experts, slots, fourth = sends.shape
    full = jax.ShapeDtypeStruct((experts, slots, fourth * n_tp), BF)
    dma = pltpu.SemaphoreType.DMA
    return pl.pallas_call(
        functools.partial(dispatch_kernel, n),
        out_shape=(full, full, jax.ShapeDtypeStruct((2, ROW_TILE, x.shape[1]), x.dtype)),
        in_specs=[VM, VM, VM],
        out_specs=(VM, VM, VM),
        scratch_shapes=[dma((2, 2, n))] * 4 + [dma((2,)), dma((2, 2))],
        compiler_params=pltpu.CompilerParams(
            collective_id=1, has_side_effects=True, vmem_limit_bytes=40 * 2**20
        ),
        cost_estimate=pl.CostEstimate(flops=0, bytes_accessed=100_000_000, transcendentals=0),
    )(sends, sendi, x)


def return_kernel(
    n, part_ref, pick_ref, out_ref, got1, got2, mid, fin, back, s_pair, s_cross, s_hop, s_tail
):
    fourth = got2.shape[2]
    slots = got2.shape[1]
    sp = lax.axis_index("sp")
    tp, partner, across, diagonal = neighbours()

    def cols(q):
        return pl.ds(pl.multiple_of(q * fourth, 128), fourth)

    greet(n)
    order = list(range(n - 1, -1, -1))
    pairs, crosses, hops = {}, {}, {}
    for d in order:
        j = partner_at(sp, n, d)
        for a, q in enumerate((diagonal, partner)):
            copy = remote(
                part_ref.at[j, :, cols(q)], got1.at[a, j], s_pair, (a, d), (sp, partner)
            )
            copy.start()
            pairs[a, d] = copy

    def stage_b(d):
        j = partner_at(sp, n, d)
        pairs[0, d].wait_recv()
        total = part_ref[j, :, cols(across)].astype(F32) + got1[0, j].astype(F32)
        mid[j] = total.astype(BF)
        copy = remote(mid.at[j], got2.at[j], s_cross, (d,), (sp, across))
        copy.start()
        crosses[d] = copy

    def stage_c(d):
        j = partner_at(sp, n, d)
        pairs[1, d].wait_recv()
        crosses[d].wait_recv()
        total = part_ref[j, :, cols(tp)].astype(F32) + got1[1, j].astype(F32)
        total = (total + got2[j].astype(F32)).astype(BF)
        if d == 0:
            back[sp] = total
        else:
            fin[j] = total
            copy = remote(fin.at[j], back.at[sp], s_hop, (d,), (j, tp))
            copy.start()
            hops[d] = copy

    lag = 2
    for i, d in enumerate(order):
        stage_b(d)
        if i >= lag:
            stage_c(order[i - lag])
    for d in order[max(n - lag, 0):]:
        stage_c(d)
    for d in range(1, n):
        hops[d].wait_recv()
    rows = back[...].reshape(n * slots, fourth)
    grad = lax.dot_general(
        pick_ref[...], rows, (((0,), (0,)), ((), ())), preferred_element_type=F32
    )
    out_ref[:, cols(tp)] = grad.astype(BF)
    own = out_ref.at[:, cols(tp)]
    over = remote(own, own, s_tail, (0,), (sp, across))
    near = remote(own, own, s_tail, (1,), (sp, partner))
    over.start()
    near.start()
    over.wait_recv()
    other = out_ref.at[:, cols(across)]
    last = remote(other, other, s_tail, (2,), (sp, partner))
    last.start()
    for d in range(n):
        for a in range(2):
            pairs[a, d].wait_send()
        crosses[d].wait_send()
        if d:
            hops[d].wait_send()
    near.wait()
    over.wait_send()
    last.wait()


def send_back(part, pick, n, n_tp):
    _, slots, width = part.shape
    fourth = width // n_tp
    dma = pltpu.SemaphoreType.DMA
    block = (n, slots, fourth)
    return pl.pallas_call(
        functools.partial(return_kernel, n),
        out_shape=jax.ShapeDtypeStruct((pick.shape[1], width), BF),
        in_specs=[VM, VM],
        out_specs=VM,
        scratch_shapes=[pltpu.VMEM((2,) + block, BF)]
        + [pltpu.VMEM(block, BF)] * 4
        + [dma((2, 2, n)), dma((2, n)), dma((2, n)), dma((2, 3))],
        compiler_params=pltpu.CompilerParams(
            collective_id=2, has_side_effects=True, vmem_limit_bytes=40 * 2**20
        ),
        cost_estimate=pl.CostEstimate(flops=0, bytes_accessed=100_000_000, transcendentals=0),
    )(part, pick)


def exchange_kernel(n, same, halo, *refs):
    if halo:
        src_ref, x_ref, dst_ref, halo_ref, sems, own, edge = refs
    else:
        src_ref, dst_ref, sems, own = refs
    sp = lax.axis_index("sp")
    tp = lax.axis_index("tp")

    def piece(i):
        return src_ref if same else src_ref.at[i]

    greet(n, with_tp=False)
    copies = list(edge_copies(n, x_ref, halo_ref, edge)) if halo else []
    local = pltpu.make_async_copy(piece(sp), dst_ref.at[sp], own.at[0])
    local.start()
    for d in range(n - 1, 0, -1):
        peer = partner_at(sp, n, d)
        copy = remote(piece(peer), dst_ref.at[sp], sems, (d,), (peer, tp))
        copy.start()
        copies.append(copy)
    local.wait()
    for copy in copies:
        copy.wait()


def exchange(x, n, same, cid, edges=None):
    out = [jax.ShapeDtypeStruct((n,) + x.shape if same else x.shape, x.dtype)]
    dma = pltpu.SemaphoreType.DMA
    scratch = [dma((2, n)), dma((1,))]
    args = [x]
    if edges is not None:
        args.append(edges)
        out.append(jax.ShapeDtypeStruct((2, ROW_TILE, edges.shape[1]), edges.dtype))
        scratch.append(dma((2, 2)))
    return pl.pallas_call(
        functools.partial(exchange_kernel, n, same, edges is not None),
        out_shape=out,
        in_specs=[VM] * len(args),
        out_specs=[VM] * len(out),
        scratch_shapes=scratch,
        compiler_params=pltpu.CompilerParams(
            collective_id=cid, has_side_effects=True, vmem_limit_bytes=24 * 2**20
        ),
        cost_estimate=pl.CostEstimate(flops=0, bytes_accessed=20_000_000, transcendentals=0),
    )(*args)


def split_dot(x, w, dims):
    high = x.astype(BF)
    rest = x - high.astype(F32)
    middle = rest.astype(BF)
    low = (rest - middle.astype(F32)).astype(BF)
    total = lax.dot_general(low, w, dims, preferred_element_type=F32)
    total = total + lax.dot_general(middle, w, dims, preferred_element_type=F32)
    return total + lax.dot_general(high, w, dims, preferred_element_type=F32)


def minus_expm1(y):
    series = 1.0 + y * (1.0 / 8.0)
    for k in (7.0, 6.0, 5.0, 4.0, 3.0, 2.0):
        series = 1.0 + y * (1.0 / k) * series
    return jnp.where(y > -0.25, -y * series, 1.0 - jnp.exp(y))


def shifted(x, by, edge):
    length = x.shape[0]
    row = lax.broadcasted_iota(jnp.int32, x.shape, 0)
    moved = pltpu.roll(x, by % length, 0)
    return jnp.where(row == (0 if by > 0 else length - 1), edge, moved)


def run_scans(length, jobs):
    width = jobs[0][1].shape[1]
    groups = length // 8

    def body(g, carry):
        out = []
        for (reverse, a_ref, b_ref, to_ref), state in zip(jobs, carry):
            base = pl.multiple_of((groups - 1 - g if reverse else g) * 8, 8)
            a = a_ref[pl.ds(base, 8), :]
            b = None if b_ref is None else b_ref[pl.ds(base, 8), :]
            rows = [None] * 8
            for k in reversed(range(8)) if reverse else range(8):
                state = a[k : k + 1] * state
                if b is not None:
                    state = state + b[k : k + 1]
                rows[k] = state
            to_ref[pl.ds(base, 8), :] = jnp.concatenate(rows, axis=0)
            out.append(state)
        return tuple(out)

    start = tuple(
        jnp.full((1, width), 1.0 if b_ref is None else 0.0, F32) for _, _, b_ref, _ in jobs
    )
    return lax.fori_loop(0, groups, body, start)


def pre_kernel(
    x_ref, low_ref, high_ref, taps_ref, maps_ref, plus_ref, shift_ref,
    conv_ref, gates_ref, decay_ref, root_ref, state_ref, cum_ref, after_ref, tot_ref, drive_ref,
):
    length, width = x_ref.shape
    taps = taps_ref[...].astype(F32)
    low = low_ref[...].astype(F32)
    high = high_ref[...].astype(F32)
    x = x_ref[...].astype(F32)
    back1 = shifted(x, 1, low[1:2])
    back2 = shifted(back1, 1, low[0:1])
    conv = back2 * taps[0:1] + back1 * taps[1:2] + x * taps[2:3]
    conv = conv + shifted(x, -1, high[0:1]) * taps[3:4]
    conv_ref[...] = conv
    gates = jax.nn.sigmoid(split_dot(conv, maps_ref[...], (((1,), (0,)), ((), ()))))
    gates_ref[...] = gates
    for d in range(2):
        recur = gates[:, 2 * d * width : (2 * d + 1) * width]
        inputs = gates[:, (2 * d + 1) * width : (2 * d + 2) * width]
        log_decay = -DECAY_SCALE * recur * plus_ref[d : d + 1, :] + shift_ref[d]
        root = jnp.sqrt(minus_expm1(2.0 * log_decay))
        decay_ref[d] = jnp.exp(log_decay)
        root_ref[d] = root
        drive_ref[d] = root * (inputs * conv)
    a_f, a_b = decay_ref.at[0], decay_ref.at[1]
    ends = run_scans(
        length,
        (
            (False, a_f, drive_ref.at[0], state_ref.at[0]),
            (True, a_b, drive_ref.at[1], state_ref.at[1]),
            (False, a_f, None, cum_ref.at[0]),
            (True, a_b, None, cum_ref.at[1]),
            (True, a_f, None, after_ref.at[0]),
            (False, a_b, None, after_ref.at[1]),
        ),
    )
    tot_ref[0:1, :] = ends[2]
    tot_ref[1:2, :] = ends[0]
    tot_ref[2:3, :] = ends[3]
    tot_ref[3:4, :] = ends[1]
    tot_ref[4:8, :] = jnp.zeros((4, width), F32)


def gelu_parts(x):
    t = jnp.tanh(GELU_K * (x + GELU_C * x * x * x))
    value = 0.5 * x * (1.0 + t)
    slope = 0.5 * (1.0 + t) + 0.5 * x * (1.0 - t * t) * GELU_K * (1.0 + 3.0 * GELU_C * x * x)
    return value, slope


def middle_kernel(
    ng_ref, cot_ref, x_ref, proj_ref, branch_ref, decay_ref, tot_ref,
    mixed_ref, out_grad_ref, carried_ref, after_ref, tot2_ref, drive_ref,
):
    length = ng_ref.shape[0]
    x = x_ref[...].astype(F32)
    inv = lax.rsqrt(jnp.mean(x * x, axis=1, keepdims=True) + EPS)
    normed = x * inv
    ng = ng_ref[...].astype(F32)
    dot = jnp.mean(ng * normed, axis=1, keepdims=True)
    mixed = (cot_ref[...].astype(F32) + inv * (ng - normed * dot)).astype(BF)
    mixed_ref[...] = mixed
    out_grad = jnp.dot(mixed, proj_ref[...], preferred_element_type=F32)
    out_grad_ref[...] = out_grad
    value, _ = gelu_parts(branch_ref[...].astype(F32))
    carried = out_grad * value
    carried_ref[...] = carried
    drive_ref[...] = decay_ref[...] * carried[None]
    ends = run_scans(
        length,
        (
            (True, decay_ref.at[0], drive_ref.at[0], after_ref.at[0]),
            (False, decay_ref.at[1], drive_ref.at[1], after_ref.at[1]),
        ),
    )
    tot2_ref[0:4, :] = tot_ref[0:4, :]
    tot2_ref[4:5, :] = ends[1]
    tot2_ref[5:6, :] = ends[0]
    tot2_ref[6:8, :] = jnp.zeros((2, tot_ref.shape[1]), F32)


def last_kernel(
    n, all_ref, conv_ref, gates_ref, decay_ref, root_ref, state_ref, cum_ref, ones_ref,
    after_ref, carried_ref, out_grad_ref, branch_ref, maps_ref, plus_ref,
    conv_grad_ref, branch_grad_ref, mixed_out_ref, packed_ref,
):
    length, width = conv_ref.shape
    sp = lax.axis_index("sp")
    zero = jnp.zeros((1, width), F32)

    def lower(k, carry):
        t = all_ref[k]
        return (t[0:1] * carry[0] + t[1:2], t[2:3] * carry[1] + t[4:5])

    def upper(i, carry):
        t = all_ref[n - 1 - i]
        return (t[2:3] * carry[0] + t[3:4], t[0:1] * carry[1] + t[5:6])

    in_f, in_ab = lax.fori_loop(0, sp, lower, (zero, zero))
    in_b, in_af = lax.fori_loop(0, n - 1 - sp, upper, (zero, zero))
    state_f = state_ref[0] + cum_ref[0] * in_f
    state_b = state_ref[1] + cum_ref[1] * in_b
    after_f = after_ref[0] + ones_ref[0] * in_af
    after_b = after_ref[1] + ones_ref[1] * in_ab
    carried = carried_ref[...]
    adjoint = (carried + shifted(after_f, -1, in_af), carried + shifted(after_b, 1, in_ab))
    beside = (shifted(state_f, 1, in_f), shifted(state_b, -1, in_b))
    conv = conv_ref[...]
    total = jnp.zeros((length, width), F32)
    for d in range(2):
        recur = gates_ref[:, 2 * d * width : (2 * d + 1) * width]
        inputs = gates_ref[:, (2 * d + 1) * width : (2 * d + 2) * width]
        decay = decay_ref[d]
        root = root_ref[d]
        g = adjoint[d]
        total = total + g * root * inputs
        g_log = g * beside[d] * decay - g * inputs * conv * (decay * decay) / root
        g_recur = g_log * (-DECAY_SCALE * plus_ref[d : d + 1, :])
        packed_ref[:, 2 * d * width : (2 * d + 1) * width] = g_recur * recur * (1.0 - recur)
        packed_ref[:, (2 * d + 1) * width : (2 * d + 2) * width] = (
            g * root * conv * inputs * (1.0 - inputs)
        )
    total = total + split_dot(packed_ref[...], maps_ref[...], (((1,), (1,)), ((), ())))
    conv_grad_ref[...] = total.astype(BF)
    value, slope = gelu_parts(branch_ref[...].astype(F32))
    states = state_f + state_b
    mixed_out_ref[...] = (value * states).astype(BF)
    branch_grad_ref[...] = (out_grad_ref[...] * states * slope).astype(BF)


def block_matrix(maps):
    heads = maps.shape[0]
    eye = jnp.eye(heads, dtype=maps.dtype)
    full = maps[:, :, None, :] * eye[:, None, :, None]
    return full.reshape(heads * maps.shape[1], heads * maps.shape[2])


def shards(
    cotangent,
    saved_input,
    routes,
    route_weight,
    gate_proj,
    up_proj,
    down_proj,
    out_proj,
    conv_input,
    gate_branch,
    conv_taps,
    recur_map,
    input_map,
    decay_param,
    decay_shift,
):
    length, width = cotangent.shape
    n = lax.axis_size("sp")
    n_tp = lax.axis_size("tp")
    experts = n * gate_proj.shape[0]
    slots = 4 * length // n
    slots = (slots + ROW_TILE - 1) // ROW_TILE * ROW_TILE
    fourth = width // n_tp
    channels = conv_input.shape[1]
    sds = jax.ShapeDtypeStruct

    sends, sendi, pick = local_call(
        functools.partial(prepare_kernel, slots),
        (cotangent, saved_input, routes.T, route_weight.T),
        (
            sds((experts, slots, fourth), BF),
            sds((experts, slots, fourth), BF),
            sds((experts * slots, length), BF),
        ),
    )
    got_scaled, got_input, halo = dispatch(sends, sendi, conv_input, n, n_tp)
    low, high = halo_edges(halo, n, 2)
    rows_scaled = got_scaled.reshape(experts * slots, width)
    rows_input = got_input.reshape(experts * slots, width)
    w_gate = gate_proj[0]
    w_up = up_proj[0]
    w_down = down_proj[0]
    gate_pre = jnp.dot(rows_input, w_gate, preferred_element_type=F32)
    up_pre = jnp.dot(rows_input, w_up, preferred_element_type=F32)
    gate_sig = jax.nn.sigmoid(gate_pre)
    gate_act = gate_pre * gate_sig
    hidden = (gate_act * up_pre).astype(BF)
    hidden_grad = lax.dot_general(
        rows_scaled, w_down, (((1,), (1,)), ((), ())), preferred_element_type=F32
    )
    gate_grad = (hidden_grad * up_pre * gate_sig * (1.0 + gate_pre * (1.0 - gate_sig))).astype(BF)
    up_grad = (hidden_grad * gate_act).astype(BF)
    partial_rows = lax.dot_general(
        gate_grad, w_gate, (((1,), (1,)), ((), ())), preferred_element_type=F32
    )
    partial_rows = partial_rows + lax.dot_general(
        up_grad, w_up, (((1,), (1,)), ((), ())), preferred_element_type=F32
    )
    part = partial_rows.astype(BF).reshape(experts, slots, width)
    normed_grad = send_back(part, pick, n, n_tp)
    rows0 = (((0,), (0,)), ((), ()))
    grad_down = lax.dot_general(hidden, rows_scaled, rows0, preferred_element_type=F32)
    grad_gate = lax.dot_general(rows_input, gate_grad, rows0, preferred_element_type=F32)
    grad_up = lax.dot_general(rows_input, up_grad, rows0, preferred_element_type=F32)

    maps = jnp.concatenate(
        [block_matrix(m[d]) for d in range(2) for m in (recur_map, input_map)], axis=1
    )
    plus = jax.nn.softplus(-decay_param)
    one = sds((length, channels), F32)
    two = sds((2, length, channels), F32)
    eight = sds((8, channels), F32)
    conv, gates, decay, root, state, cum, ones, tot, _ = local_call(
        pre_kernel,
        (conv_input, low, high, conv_taps, maps, plus, decay_shift),
        (one, sds((length, 4 * channels), F32), two, two, two, two, two, eight, two),
    )
    mixed_grad_b, out_grad, carried, after, tot2, _ = local_call(
        middle_kernel,
        (normed_grad, cotangent, saved_input, out_proj, gate_branch, decay, tot),
        (sds((length, width), BF), one, one, two, eight, two),
    )
    (everyone,) = exchange(tot2, n, True, 3)
    conv_grad, branch_grad, mixed_out, _ = local_call(
        functools.partial(last_kernel, n),
        (
            everyone, conv, gates, decay, root, state, cum, ones, after, carried, out_grad,
            gate_branch, maps, plus,
        ),
        (
            sds((length, channels), BF),
            sds((length, channels), BF),
            sds((length, channels), BF),
            sds((length, 4 * channels), F32),
        ),
    )
    grad_part = lax.dot_general(mixed_grad_b, mixed_out, rows0, preferred_element_type=F32)
    pieces, grad_halo = exchange(
        grad_part.astype(BF).reshape(n, width // n, channels), n, False, 4, conv_grad
    )
    grad_low, grad_high = halo_edges(grad_halo, n, 2)
    grad_out = jnp.sum(pieces.astype(F32), axis=0)
    taps32 = conv_taps.astype(F32)
    grad_pad = jnp.concatenate([grad_low, conv_grad, grad_high], axis=0).astype(F32)
    input_grad = jnp.zeros((length, channels), F32)
    for offset in range(taps32.shape[0]):
        input_grad = input_grad + grad_pad[4 - offset : 4 - offset + length] * taps32[offset]
    return (
        grad_gate[None],
        grad_up[None],
        grad_down[None],
        grad_out,
        input_grad.astype(BF),
        branch_grad,
    )


def solution(mesh):
    in_specs = (
        P("sp", None),
        P("sp", None),
        P("sp", None),
        P("sp", None),
        P("sp", None, "tp"),
        P("sp", None, "tp"),
        P("sp", "tp", None),
        P(None, "tp"),
        P("sp", "tp"),
        P("sp", "tp"),
        P(None, "tp"),
        P(None, "tp", None, None),
        P(None, "tp", None, None),
        P(None, "tp"),
        P(None, "sp", "tp"),
    )
    out_specs = (
        P("sp", None, "tp"),
        P("sp", None, "tp"),
        P("sp", "tp", None),
        P("sp", "tp"),
        P("sp", "tp"),
        P("sp", "tp"),
    )
    return jax.shard_map(shards, mesh=mesh, in_specs=in_specs, out_specs=out_specs, check_vma=False)
```
